32 devices in a mesh: sp: 8 (over z, y), dp: 4 (over x, core).
Axes of the slice: x: 2, y: 2, z: 4, core: 2. Of those that a mesh axis runs over, the one named last changes fastest.
Arguments:
- queries: bfloat16 [4, 1024, 2048], P('dp', 'sp'), may hold values from -40 to 40
- keys: bfloat16 [4, 1024, 512], P('dp', 'sp'), may hold values from -8 to 8
- values: bfloat16 [4, 1024, 512], P('dp', 'sp'), may hold values from -6 to 6
- lambdas: float32 [16], replicated, may hold values from 0.3 to 0.8
- value_gain: float32 [128], replicated, may hold values from 0.1 to 1.9
- out_weight: bfloat16 [2048, 4096], P(None, ('sp', 'dp')), may hold values from -0.125 to 0.125
Outputs:
- mixed: bfloat16 [4, 1024, 4096], P('dp', 'sp')
The draws below stay inside these ranges and needn't reach their ends.
All inputs are finite; a program needn't handle non-finite values.
Results may differ from the reference program's by a relative error of at most 0.0087.
Values may be sent and summed in bfloat16 or wider, within the bound.
A program may use at most 128 MiB of HBM per device.

```python
import jax
import jax.numpy as jnp
from jax import lax

D = 4096
HEADS = 16
KV_HEADS = 4
HEAD_DIM = 64
VALUE_DIM = 128
SEQLEN = 1024
SEQS = 4


def base_keys(key):
    draw_key = jax.random.fold_in(key, 3)
    shape = (SEQS, SEQLEN, KV_HEADS, 2, HEAD_DIM)
    keys_float = jnp.clip(1.3 * jax.random.normal(draw_key, shape, jnp.float32), -8.0, 8.0)
    return keys_float


def draw_keys(key, part):
    return base_keys(key).reshape(SEQS, SEQLEN, KV_HEADS * 2 * HEAD_DIM).astype(jnp.bfloat16)


def draw_queries(key, part):
    draw_key = jax.random.fold_in(key, 4)
    shape = (SEQS, SEQLEN, HEADS, 2, HEAD_DIM)
    queries_float = jnp.clip(1.3 * jax.random.normal(draw_key, shape, jnp.float32), -8.0, 8.0)
    return queries_float.reshape(SEQS, SEQLEN, HEADS * 2 * HEAD_DIM).astype(jnp.bfloat16)


def block_levels(own_key, shape, pieces, low, high):
    loudness = 1.0
    for position, blocks in pieces:
        steps = jax.random.uniform(jax.random.fold_in(jax.random.fold_in(own_key, 6), position), (blocks,), jnp.float32, low / len(pieces), high / len(pieces))
        loudness = loudness * jnp.repeat(jnp.exp(steps), shape[position] // blocks).reshape((-1,) + (1,) * (len(shape) - 1 - position))
    return loudness


def scatter_about(own_key, extent, deviation, most, split=(), kind=jnp.bfloat16):
    result = deviation * jax.random.normal(own_key, extent, jnp.float32)
    if split:
        result = result * block_levels(own_key, extent, split, -0.22, 0.18)
    return jnp.clip(result, -most, most).astype(kind)


def setup_inputs(seed: int = 0) -> dict:
    key_of = jax.random.split(jax.random.key(seed), 7)
    queries = draw_queries(jax.random.fold_in(key_of[6], 71), 0)
    keys = draw_keys(jax.random.fold_in(key_of[6], 71), 0)
    values = scatter_about(key_of[2], (SEQS, SEQLEN, KV_HEADS * VALUE_DIM), 1.0, 6.0, ((0, 4), (1, 8)))
    lambdas = jnp.clip(jax.random.uniform(key_of[3], (HEADS,), jnp.float32, 0.3, 0.8), 0.3, 0.8)
    value_gain = jnp.clip(1.0 + 0.18 * jax.random.normal(key_of[4], (VALUE_DIM,), jnp.float32), 0.1, 1.9)
    out_weight = scatter_about(key_of[5], (HEADS * VALUE_DIM, D), (HEADS * VALUE_DIM) ** -0.5, 0.125, ((1, 32),))
    return {"queries": queries, "keys": keys, "values": values, "lambdas": lambdas, "value_gain": value_gain, "out_weight": out_weight}


rope_base = 500000.0
output_scale = 0.8
norm_eps = 1e-05

def rotate_all(parts, positions):
    width = parts.shape[-1]
    half = width // 2
    freqs = rope_base ** (-jnp.arange(0, width, 2, dtype=jnp.float32) / width)
    angles = positions[:, None] * freqs[None, :]
    shape = (1, angles.shape[0], 1, 1, half)
    cosine = jnp.cos(angles).reshape(shape)
    sine = jnp.sin(angles).reshape(shape)
    first = parts[..., :half]
    second = parts[..., half:]
    return jnp.concatenate([first * cosine - second * sine, second * cosine + first * sine], -1)

def reference(queries, keys, values, lambdas, value_gain, out_weight):
    positions = jnp.arange(SEQLEN, dtype=jnp.float32)
    query_rot = rotate_all(queries.astype(jnp.float32).reshape(SEQS, SEQLEN, HEADS, 2, HEAD_DIM), positions).astype(jnp.bfloat16)
    key_rot = rotate_all(keys.astype(jnp.float32).reshape(SEQS, SEQLEN, KV_HEADS, 2, HEAD_DIM), positions).astype(jnp.bfloat16)
    value_parts = values.reshape(SEQS, SEQLEN, KV_HEADS, VALUE_DIM)
    group_size = HEADS // KV_HEADS
    key_heads = jnp.repeat(key_rot, group_size, axis=2)
    value_heads = jnp.repeat(value_parts, group_size, axis=2)
    query_flat = jnp.transpose(query_rot, (0, 2, 1, 3, 4)).reshape(SEQS * HEADS, SEQLEN, 2, HEAD_DIM)
    key_flat = jnp.transpose(key_heads, (0, 2, 1, 3, 4)).reshape(SEQS * HEADS, SEQLEN, 2, HEAD_DIM)
    value_flat = jnp.transpose(value_heads, (0, 2, 1, 3)).reshape(SEQS * HEADS, SEQLEN, VALUE_DIM)
    lambda_flat = jnp.tile(lambdas, SEQS)
    block_rows = min(512, SEQLEN)
    count = SEQLEN // block_rows
    score_scale = HEAD_DIM ** (-0.5)
    key_places = jnp.arange(SEQLEN)

    def one_head(inputs):
        query_one, key_one, value_one, lambda_one = inputs

        def one_block(block_index):
            start = block_index * block_rows
            query_block = lax.dynamic_slice_in_dim(query_one, start, block_rows, 0)
            scores = jnp.einsum('qmd,kmd->mqk', query_block.astype(jnp.float32), key_one.astype(jnp.float32)) * score_scale
            allowed = key_places[None, :] <= (start + jnp.arange(block_rows))[:, None]
            scores = jnp.where(allowed[None], scores, -jnp.inf)
            row_top = lax.optimization_barrier(jnp.max(scores, -1, keepdims=True))
            raised = jnp.exp(scores - row_top)
            maps = raised / lax.optimization_barrier(jnp.sum(raised, -1, keepdims=True))
            weights = (maps[0] - lambda_one * maps[1]).astype(jnp.bfloat16)
            return jnp.dot(weights, value_one, preferred_element_type=jnp.float32)
        blocks = lax.map(one_block, jnp.arange(count))
        head_values = blocks.reshape(SEQLEN, VALUE_DIM)
        squares = lax.optimization_barrier(jnp.mean(head_values * head_values, -1, keepdims=True))
        return (head_values * lax.rsqrt(squares + norm_eps) * value_gain * output_scale).astype(jnp.bfloat16)
    head_out = lax.map(one_head, (query_flat, key_flat, value_flat, lambda_flat))
    heads_out = jnp.transpose(head_out.reshape(SEQS, HEADS, SEQLEN, VALUE_DIM), (0, 2, 1, 3)).reshape(SEQS * SEQLEN, HEADS * VALUE_DIM)
    mixed = jnp.dot(heads_out, out_weight, preferred_element_type=jnp.float32).astype(jnp.bfloat16)
    return mixed.reshape(SEQS, SEQLEN, D)
```

```python
import functools

import jax
import jax.numpy as jnp
from jax import lax
from jax.experimental import pallas as pl
from jax.experimental.pallas import tpu as pltpu
from jax.sharding import PartitionSpec as P

HEADS = 16
KV_HEADS = 4
HEAD_DIM = 64
VALUE_DIM = 128
GROUP = HEADS // KV_HEADS

rope_base = 500000.0
output_scale = 0.8
norm_eps = 1e-05
MESH = pl.DeviceIdType.MESH


def tables(positions):
    freqs = rope_base ** (-jnp.arange(0, HEAD_DIM, 2, dtype=jnp.float32) / HEAD_DIM)
    angles = positions[:, None] * freqs[None, :]
    cosine, sine = jnp.cos(angles), jnp.sin(angles)
    return jnp.concatenate([cosine] * 4, -1), jnp.concatenate([-sine, sine, -sine, sine], -1)


def turn(block, cosine, sine):
    half = HEAD_DIM // 2
    lane = lax.broadcasted_iota(jnp.int32, block.shape, 1)
    other = jnp.where(
        lane % HEAD_DIM < half,
        pltpu.roll(block, block.shape[1] - half, 1),
        pltpu.roll(block, half, 1),
    )
    return block * cosine + other * sine


def prep_kernel(k_ref, v_ref, cos_ref, sin_ref, kv_ref):
    width = 2 * HEAD_DIM
    for g in range(KV_HEADS):
        cols = slice(g * width, (g + 1) * width)
        kv_ref[:, cols] = turn(
            k_ref[:, cols].astype(jnp.float32), cos_ref[...], sin_ref[...]
        ).astype(jnp.bfloat16)
    kv_ref[:, KV_HEADS * width :] = v_ref[...]


def attend_kernel(lam_ref, q_ref, k_ref, v_ref, cos_ref, sin_ref, gain_ref, out_ref):
    rows, seqlen = q_ref.shape[0], k_ref.shape[0]
    g = pl.program_id(0)
    width = 2 * HEAD_DIM
    start = lax.axis_index("sp") * rows
    allowed = lax.broadcasted_iota(jnp.int32, (rows, seqlen), 1) <= (
        start + lax.broadcasted_iota(jnp.int32, (rows, seqlen), 0)
    )
    lane = lax.broadcasted_iota(jnp.int32, (rows, width), 1)
    gain = gain_ref[...]
    for h in range(GROUP):
        cols = slice(h * width, (h + 1) * width)
        query = turn(q_ref[:, cols].astype(jnp.float32), cos_ref[...], sin_ref[...])
        query = query.astype(jnp.bfloat16).astype(jnp.float32) * HEAD_DIM**-0.5
        maps = []
        for m in range(2):
            own = (lane < HEAD_DIM) if m == 0 else (lane >= HEAD_DIM)
            part = jnp.where(own, query, 0.0).astype(jnp.bfloat16)
            scores = lax.dot_general(
                part, k_ref[...], (((1,), (1,)), ((), ())), preferred_element_type=jnp.float32
            )
            scores = jnp.where(allowed, scores, -1e30)
            raised = jnp.exp(scores - jnp.max(scores, -1, keepdims=True))
            maps.append((raised, 1.0 / jnp.sum(raised, -1, keepdims=True)))
        lam = lam_ref[g * GROUP + h]
        weights = (
            maps[0][0] * maps[0][1] - maps[1][0] * (lam * maps[1][1])
        ).astype(jnp.bfloat16)
        value = jnp.dot(weights, v_ref[...], preferred_element_type=jnp.float32)
        squares = jnp.mean(value * value, -1, keepdims=True)
        normed = value * lax.rsqrt(squares + norm_eps) * gain * output_scale
        out_ref[:, cols] = normed.astype(jnp.bfloat16)


def send(src, dst, send_sem, recv_sem, dp):
    return pltpu.make_async_remote_copy(
        src_ref=src,
        dst_ref=dst,
        send_sem=send_sem,
        recv_sem=recv_sem,
        device_id={"dp": dp},
        device_id_type=MESH,
    )


def exchange_kernel(count, heads_ref, all_ref, own_sem, send_sems, recv_sems, fs_sems, fr_sems):
    d = lax.axis_index("dp")
    half = count // 2
    x, core = d // 2, d % 2
    mate = x * 2 + 1 - core
    barrier = pltpu.get_barrier_semaphore()
    pl.semaphore_signal(barrier, inc=1, device_id={"dp": mate}, device_id_type=MESH)
    for k in range(1, half):
        pl.semaphore_signal(
            barrier, inc=1, device_id={"dp": (x + k) % half * 2 + core}, device_id_type=MESH
        )
    pl.semaphore_wait(barrier, half)
    copies = []
    for k in range(1, half):
        copies.append(
            send(heads_ref, all_ref.at[d], send_sems.at[k], recv_sems.at[k], (x + k) % half * 2 + core)
        )
        copies[-1].start()
    first = send(heads_ref, all_ref.at[d], send_sems.at[0], recv_sems.at[0], mate)
    first.start()
    local = pltpu.make_async_copy(heads_ref, all_ref.at[d], own_sem)
    local.start()
    forwards = []
    for k in range(1, half):
        slot = all_ref.at[(x + half - k) % half * 2 + core]
        copies[k - 1].wait_recv()
        forwards.append(send(slot, slot, fs_sems.at[k], fr_sems.at[k], mate))
        forwards[-1].start()
    local.wait()
    first.wait()
    for copy in copies:
        copy.wait_send()
    for copy in forwards:
        copy.wait()


def project_kernel(count, per, heads_ref, w_ref, out_ref, built, send_sems, recv_sems):
    d = lax.axis_index("dp")
    barrier = pltpu.get_barrier_semaphore()
    for k in range(1, count):
        pl.semaphore_signal(barrier, inc=1, device_id={"dp": (d + k) % count}, device_id_type=MESH)
    rows, depth = heads_ref.shape[1:]
    heads = heads_ref[...].reshape(count * rows, depth)
    chunks = out_ref.shape[0]
    copies = []
    for j in range(chunks):
        weight = jnp.concatenate([w_ref[j * per + i] for i in range(per)], -1)
        mixed = jnp.dot(heads, weight, preferred_element_type=jnp.float32).astype(jnp.bfloat16)
        built[j] = mixed.reshape(count, rows, -1)
        if j == 0:
            pl.semaphore_wait(barrier, count - 1)
        for k in range(1, count):
            copies.append(
                send(
                    built.at[j, (d + k) % count],
                    out_ref.at[j, d],
                    send_sems.at[j, k],
                    recv_sems.at[j, k],
                    (d + k) % count,
                )
            )
            copies[-1].start()
        out_ref[j, d] = built[j, d]
    for copy in copies:
        copy.wait()


def shards(queries, keys, values, lambdas, value_gain, out_weight):
    rows = queries.shape[1]
    sp_count = lax.axis_size("sp")
    dp_count = lax.axis_size("dp")
    seqlen = rows * sp_count
    width = 2 * HEAD_DIM
    vmem = pl.BlockSpec(memory_space=pltpu.VMEM)
    bf16 = jnp.bfloat16
    positions = (lax.axis_index("sp") * rows + jnp.arange(rows)).astype(jnp.float32)
    cosine, sine = tables(positions)

    kv = pl.pallas_call(
        prep_kernel,
        out_shape=jax.ShapeDtypeStruct((rows, 2 * KV_HEADS * width), bf16),
        in_specs=[vmem] * 4,
        out_specs=vmem,
        name="prep",
    )(keys[0], values[0], cosine, sine)
    kv_whole = lax.all_gather(kv, "sp", axis=0, tiled=True)
    kv_whole, out_weight = lax.optimization_barrier((kv_whole, out_weight))
    weights = lax.all_gather(out_weight, "sp", axis=0)

    heads = pl.pallas_call(
        attend_kernel,
        grid=(KV_HEADS,),
        out_shape=jax.ShapeDtypeStruct((rows, HEADS * VALUE_DIM), bf16),
        in_specs=[
            pl.BlockSpec(memory_space=pltpu.SMEM),
            pl.BlockSpec((rows, GROUP * width), lambda g: (0, g)),
            pl.BlockSpec((seqlen, width), lambda g: (0, g)),
            pl.BlockSpec((seqlen, VALUE_DIM), lambda g: (0, KV_HEADS + g)),
            pl.BlockSpec((rows, width), lambda g: (0, 0)),
            pl.BlockSpec((rows, width), lambda g: (0, 0)),
            pl.BlockSpec((1, VALUE_DIM), lambda g: (0, 0)),
        ],
        out_specs=pl.BlockSpec((rows, GROUP * VALUE_DIM), lambda g: (0, g)),
        cost_estimate=pl.CostEstimate(
            flops=3 * 10**9, bytes_accessed=4 * 2**20, transcendentals=4 * 2**20
        ),
        name="attend",
    )(lambdas, queries[0], kv_whole, kv_whole, cosine, sine, value_gain[None])

    half = dp_count // 2
    dma = pltpu.SemaphoreType.DMA
    heads_all = pl.pallas_call(
        functools.partial(exchange_kernel, dp_count),
        out_shape=jax.ShapeDtypeStruct((dp_count, rows, HEADS * VALUE_DIM), bf16),
        in_specs=[vmem],
        out_specs=vmem,
        scratch_shapes=[dma(())] + [dma((half,))] * 4,
        compiler_params=pltpu.CompilerParams(collective_id=0, has_side_effects=True),
        cost_estimate=pl.CostEstimate(flops=0, bytes_accessed=32 * 2**20, transcendentals=0),
        name="exchange",
    )(heads)

    own = out_weight.shape[1]
    depth = out_weight.shape[0]
    block = min(256, sp_count * own)
    if own % 128:
        weights = jnp.transpose(weights, (1, 0, 2)).reshape(depth, -1, block)
        weights = jnp.transpose(weights, (1, 0, 2))
    per = max(1, block // weights.shape[2])
    chunks = weights.shape[0] // per
    block = per * weights.shape[2]
    mixed = pl.pallas_call(
        functools.partial(project_kernel, dp_count, per),
        out_shape=jax.ShapeDtypeStruct((chunks, dp_count, rows, block), bf16),
        in_specs=[vmem] * 2,
        out_specs=vmem,
        scratch_shapes=[
            pltpu.VMEM((chunks, dp_count, rows, block), bf16),
            dma((chunks, dp_count)),
            dma((chunks, dp_count)),
        ],
        compiler_params=pltpu.CompilerParams(collective_id=1, has_side_effects=True),
        name="project",
    )(heads_all, weights)
    mixed = mixed.reshape(chunks, dp_count, rows, block // own, own)
    mixed = jnp.transpose(mixed, (2, 0, 3, 1, 4))
    return mixed.reshape(1, rows, -1)


def solution(mesh):
    return jax.shard_map(
        shards,
        mesh=mesh,
        in_specs=(
            P("dp", "sp", None),
            P("dp", "sp", None),
            P("dp", "sp", None),
            P(),
            P(),
            P(None, ("sp", "dp")),
        ),
        out_specs=P("dp", "sp", None),
        check_vma=False,
    )
```

```python
import functools

import jax
import jax.numpy as jnp
from jax import lax
from jax.experimental import pallas as pl
from jax.experimental.pallas import tpu as pltpu
from jax.sharding import PartitionSpec as P

HEADS = 16
KV_HEADS = 4
HEAD_DIM = 64
VALUE_DIM = 128
GROUP = HEADS // KV_HEADS

rope_base = 500000.0
output_scale = 0.8
norm_eps = 1e-05
MESH = pl.DeviceIdType.MESH


def tables(positions):
    freqs = rope_base ** (-jnp.arange(0, HEAD_DIM, 2, dtype=jnp.float32) / HEAD_DIM)
    angles = positions[:, None] * freqs[None, :]
    cosine, sine = jnp.cos(angles), jnp.sin(angles)
    return jnp.concatenate([cosine] * 4, -1), jnp.concatenate([-sine, sine, -sine, sine], -1)


def turn(block, cosine, sine):
    half = HEAD_DIM // 2
    lane = lax.broadcasted_iota(jnp.int32, block.shape, 1)
    other = jnp.where(
        lane % HEAD_DIM < half,
        pltpu.roll(block, block.shape[1] - half, 1),
        pltpu.roll(block, half, 1),
    )
    return block * cosine + other * sine


def prep_kernel(k_ref, v_ref, cos_ref, sin_ref, kv_ref):
    width = 2 * HEAD_DIM
    for g in range(KV_HEADS):
        cols = slice(g * width, (g + 1) * width)
        kv_ref[:, cols] = turn(
            k_ref[:, cols].astype(jnp.float32), cos_ref[...], sin_ref[...]
        ).astype(jnp.bfloat16)
    kv_ref[:, KV_HEADS * width :] = v_ref[...]


def send(src, dst, send_sem, recv_sem, axis, index):
    return pltpu.make_async_remote_copy(
        src_ref=src,
        dst_ref=dst,
        send_sem=send_sem,
        recv_sem=recv_sem,
        device_id={axis: index},
        device_id_type=MESH,
    )


def layer_kernel(
    n,
    count,
    lam_ref,
    q_ref,
    kv_ref,
    cos_ref,
    sin_ref,
    gain_ref,
    w_ref,
    out_ref,
    kv_all,
    w_all,
    heads_all,
    built,
    own_sem,
    kv_send,
    kv_recv,
    w_send,
    w_recv,
    x_send,
    x_recv,
    mate_send,
    mate_recv,
    out_send,
    out_recv,
):
    bf16 = jnp.bfloat16
    d = lax.axis_index("dp")
    me = lax.axis_index("sp")
    half = count // 2
    tall = n // half
    steps = n // 2
    width = 2 * HEAD_DIM
    rows = q_ref.shape[0]
    seqlen = n * rows

    def flip(column, place):
        return place + column % 2 * (tall - 1 - 2 * place)

    pos = me % half * tall + flip(me % half, me // half)

    def at(place):
        place = (place + 2 * n) % n
        column = place // tall
        return flip(column, place % tall) * half + column

    ahead, behind = at(pos + 1), at(pos - 1)
    x, core = d // 2, d % 2
    mate = x * 2 + 1 - core

    def peer(k):
        return (x + k) % half * 2 + core

    barrier = pltpu.get_barrier_semaphore()
    for other in (ahead, behind):
        pl.semaphore_signal(barrier, inc=1, device_id={"sp": other}, device_id_type=MESH)
    for k in range(1, count):
        pl.semaphore_signal(barrier, inc=1, device_id={"dp": (d + k) % count}, device_id_type=MESH)
    pl.semaphore_wait(barrier, count + 1)

    def ring_step(own, held, sends, recvs, t):
        pair = []
        for way in range(2):
            slot = at(pos - (t - 1)) if way == 0 else at(pos + (t - 1))
            src = own if t == 1 else held.at[slot]
            dst = held.at[slot]
            if t == steps:
                cut = held.shape[1] // 2
                part = pl.ds(way * cut, cut)
                src, dst = src.at[part], dst.at[part]
            pair.append(
                send(src, dst, sends.at[way, t - 1], recvs.at[way, t - 1], "sp", behind if way else ahead)
            )
            pair[-1].start()
        return pair

    kv_pairs = [ring_step(kv_ref, kv_all, kv_send, kv_recv, 1)]
    local = pltpu.make_async_copy(kv_ref, kv_all.at[me], own_sem)
    local.start()
    w_pairs = []
    for t in range(1, steps + 1):
        for copy in kv_pairs[t - 1]:
            copy.wait_recv()
        if t < steps:
            kv_pairs.append(ring_step(kv_ref, kv_all, kv_send, kv_recv, t + 1))
        if t == steps - 1:
            w_pairs.append(ring_step(w_ref, w_all, w_send, w_recv, 1))
    local.wait()

    allowed = lax.broadcasted_iota(jnp.int32, (rows, seqlen), 1) <= (
        me * rows + lax.broadcasted_iota(jnp.int32, (rows, seqlen), 0)
    )
    lane = lax.broadcasted_iota(jnp.int32, (rows, width), 1)

    def span(g):
        return pl.ds(pl.multiple_of(g * GROUP * VALUE_DIM, GROUP * VALUE_DIM), GROUP * VALUE_DIM)

    def sends_of(g):
        part = heads_all.at[d, :, span(g)]
        result = [send(part, part, x_send.at[0, g], x_recv.at[0, g], "dp", mate)]
        for k in range(1, half):
            result.append(send(part, part, x_send.at[k, g], x_recv.at[k, g], "dp", peer(k)))
        return result

    def one_group(g, carry):
        key = kv_all[:, :, pl.ds(pl.multiple_of(g * width, width), width)]
        key = key.reshape(seqlen, width)
        start = pl.multiple_of(KV_HEADS * width + g * VALUE_DIM, VALUE_DIM)
        value = kv_all[:, :, pl.ds(start, VALUE_DIM)].reshape(seqlen, VALUE_DIM)
        for h in range(GROUP):
            column = pl.multiple_of((g * GROUP + h) * width, width)
            query = q_ref[:, pl.ds(column, width)].astype(jnp.float32)
            query = turn(query, cos_ref[...], sin_ref[...]).astype(bf16)
            query = query.astype(jnp.float32) * HEAD_DIM**-0.5
            maps = []
            for m in range(2):
                mine = (lane < HEAD_DIM) if m == 0 else (lane >= HEAD_DIM)
                part = jnp.where(mine, query, 0.0).astype(bf16)
                scores = lax.dot_general(
                    part, key, (((1,), (1,)), ((), ())), preferred_element_type=jnp.float32
                )
                scores = jnp.where(allowed, scores, -1e30)
                raised = jnp.exp(scores - jnp.max(scores, -1, keepdims=True))
                maps.append((raised, 1.0 / jnp.sum(raised, -1, keepdims=True)))
            lam = lam_ref[g * GROUP + h]
            weights = (
                maps[0][0] * maps[0][1] - maps[1][0] * (lam * maps[1][1])
            ).astype(bf16)
            found = jnp.dot(weights, value, preferred_element_type=jnp.float32)
            squares = jnp.mean(found * found, -1, keepdims=True)
            normed = found * lax.rsqrt(squares + norm_eps) * gain_ref[...] * output_scale
            heads_all[d, :, pl.ds(column, width)] = normed.astype(bf16)
        for copy in sends_of(g):
            copy.start()
        return carry

    lax.fori_loop(0, KV_HEADS, one_group, 0)

    def weights_step(t):
        for copy in w_pairs[t - 1]:
            copy.wait_recv()
        if t < steps:
            w_pairs.append(ring_step(w_ref, w_all, w_send, w_recv, t + 1))

    weights_step(1)

    forwards = []
    for g in range(KV_HEADS):
        copies = sends_of(g)
        for k in range(1, half):
            copies[k].wait_recv()
            part = heads_all.at[(x + half - k) % half * 2 + core, :, span(g)]
            forwards.append(
                send(part, part, mate_send.at[k, g], mate_recv.at[k, g], "dp", mate)
            )
            forwards[-1].start()
    for g in range(KV_HEADS):
        sends_of(g)[0].wait_recv()
    for copy in forwards:
        copy.wait_recv()

    heads = heads_all[...].reshape(count * rows, heads_all.shape[2])
    own = w_ref.shape[1]
    outs = []
    for t in range(1, steps + 1):
        if t > 1:
            weights_step(t)
        places = (pos - t, pos + t) if t < steps else (pos, pos + steps)
        slots = [at(place) for place in places]
        blocks = [
            w_ref[...] if t == steps and i == 0 else w_all[slots[i]] for i in range(2)
        ]
        if own % 128 == 0:
            both = jnp.concatenate(blocks, -1)
            both = jnp.dot(heads, both, preferred_element_type=jnp.float32).astype(bf16)
            results = [both[:, :own], both[:, own:]]
        else:
            results = [
                jnp.dot(heads, block, preferred_element_type=jnp.float32).astype(bf16)
                for block in blocks
            ]
        for i in range(2):
            built[t - 1, i] = results[i].reshape(count, rows, own)
        for k in range(1, count):
            to = (d + k) % count
            for i in range(2):
                outs.append(
                    send(
                        built.at[t - 1, i, to],
                        out_ref.at[slots[i], d],
                        out_send.at[t - 1, i, k],
                        out_recv.at[t - 1, i, k],
                        "dp",
                        to,
                    )
                )
                outs[-1].start()
        for i in range(2):
            out_ref[slots[i], d] = built[t - 1, i, d]
    for copy in outs:
        copy.wait()
    for pair in kv_pairs + w_pairs:
        for copy in pair:
            copy.wait_send()
    for g in range(KV_HEADS):
        for copy in sends_of(g):
            copy.wait_send()
    for copy in forwards:
        copy.wait_send()


def lay_kernel(in_ref, out_ref):
    own = in_ref.shape[2]
    for b in range(in_ref.shape[0]):
        out_ref[:, b * own : (b + 1) * own] = in_ref[b]


def shards(queries, keys, values, lambdas, value_gain, out_weight):
    rows = queries.shape[1]
    sp_count = lax.axis_size("sp")
    dp_count = lax.axis_size("dp")
    width = 2 * HEAD_DIM
    vmem = pl.BlockSpec(memory_space=pltpu.VMEM)
    bf16 = jnp.bfloat16
    positions = (lax.axis_index("sp") * rows + jnp.arange(rows)).astype(jnp.float32)
    cosine, sine = tables(positions)
    kv_width = 2 * KV_HEADS * width

    kv = pl.pallas_call(
        prep_kernel,
        out_shape=jax.ShapeDtypeStruct((rows, kv_width), bf16),
        in_specs=[vmem] * 4,
        out_specs=vmem,
        name="prep",
    )(keys[0], values[0], cosine, sine)

    half = dp_count // 2
    steps = sp_count // 2
    depth, own = out_weight.shape
    dma = pltpu.SemaphoreType.DMA
    mixed = pl.pallas_call(
        functools.partial(layer_kernel, sp_count, dp_count),
        out_shape=jax.ShapeDtypeStruct((sp_count, dp_count, rows, own), bf16),
        in_specs=[pl.BlockSpec(memory_space=pltpu.SMEM)] + [vmem] * 6,
        out_specs=vmem,
        scratch_shapes=[
            pltpu.VMEM((sp_count, rows, kv_width), bf16),
            pltpu.VMEM((sp_count, depth, own), bf16),
            pltpu.VMEM((dp_count, rows, depth), bf16),
            pltpu.VMEM((steps, 2, dp_count, rows, own), bf16),
            dma(()),
        ]
        + [dma((2, steps))] * 4
        + [dma((half, KV_HEADS))] * 4
        + [dma((steps, 2, dp_count))] * 2,
        compiler_params=pltpu.CompilerParams(
            collective_id=0, has_side_effects=True, vmem_limit_bytes=60 * 2**20
        ),
        name="layer",
    )(lambdas, queries[0], kv, cosine, sine, value_gain[None], out_weight)

    if own % 128 == 0:
        return pl.pallas_call(
            lay_kernel,
            out_shape=jax.ShapeDtypeStruct((rows, sp_count * dp_count * own), bf16),
            in_specs=[vmem],
            out_specs=vmem,
            name="lay",
        )(mixed.reshape(-1, rows, own))[None]
    return jnp.transpose(mixed, (2, 0, 1, 3)).reshape(1, rows, -1)


def solution(mesh):
    return jax.shard_map(
        shards,
        mesh=mesh,
        in_specs=(
            P("dp", "sp", None),
            P("dp", "sp", None),
            P("dp", "sp", None),
            P(),
            P(),
            P(None, ("sp", "dp")),
        ),
        out_specs=P("dp", "sp", None),
        check_vma=False,
    )
```

```python
import functools

import jax
import jax.numpy as jnp
from jax import lax
from jax.experimental import pallas as pl
from jax.experimental.pallas import tpu as pltpu
from jax.sharding import PartitionSpec as P

HEADS = 16
KV_HEADS = 4
HEAD_DIM = 64
VALUE_DIM = 128
GROUP = HEADS // KV_HEADS

rope_base = 500000.0
output_scale = 0.8
norm_eps = 1e-05
MESH = pl.DeviceIdType.MESH


def tables(positions):
    freqs = rope_base ** (-jnp.arange(0, HEAD_DIM, 2, dtype=jnp.float32) / HEAD_DIM)
    angles = positions[:, None] * freqs[None, :]
    cosine, sine = jnp.cos(angles), jnp.sin(angles)
    return jnp.concatenate([cosine] * 4, -1), jnp.concatenate([-sine, sine, -sine, sine], -1)


def turn(block, cosine, sine):
    half = HEAD_DIM // 2
    lane = lax.broadcasted_iota(jnp.int32, block.shape, 1)
    other = jnp.where(
        lane % HEAD_DIM < half,
        pltpu.roll(block, block.shape[1] - half, 1),
        pltpu.roll(block, half, 1),
    )
    return block * cosine + other * sine


def send(src, dst, send_sem, recv_sem, axis, index):
    return pltpu.make_async_remote_copy(
        src_ref=src,
        dst_ref=dst,
        send_sem=send_sem,
        recv_sem=recv_sem,
        device_id={axis: index},
        device_id_type=MESH,
    )


def layer_kernel(
    n,
    count,
    lam_ref,
    q_ref,
    k_ref,
    v_ref,
    cos_ref,
    sin_ref,
    gain_ref,
    w_ref,
    out_ref,
    kv_own,
    kv_all,
    w_all,
    heads_all,
    built,
    own_sem,
    kv_send,
    kv_recv,
    w_send,
    w_recv,
    x_send,
    x_recv,
    mate_send,
    mate_recv,
    out_send,
    out_recv,
):
    bf16 = jnp.bfloat16
    d = lax.axis_index("dp")
    me = lax.axis_index("sp")
    half = count // 2
    tall = n // half
    steps = n // 2
    width = 2 * HEAD_DIM
    rows = q_ref.shape[0]
    seqlen = n * rows

    def flip(column, place):
        return place + column % 2 * (tall - 1 - 2 * place)

    pos = me % half * tall + flip(me % half, me // half)

    def at(place):
        place = (place + 2 * n) % n
        column = place // tall
        return flip(column, place % tall) * half + column

    ahead, behind = at(pos + 1), at(pos - 1)
    x, core = d // 2, d % 2
    mate = x * 2 + 1 - core

    def peer(k):
        return (x + k) % half * 2 + core

    barrier = pltpu.get_barrier_semaphore()
    for other in (ahead, behind):
        pl.semaphore_signal(barrier, inc=1, device_id={"sp": other}, device_id_type=MESH)
    for k in range(1, count):
        pl.semaphore_signal(barrier, inc=1, device_id={"dp": (d + k) % count}, device_id_type=MESH)
    for g in range(KV_HEADS):
        cols = slice(g * width, (g + 1) * width)
        key = turn(k_ref[:, cols].astype(jnp.float32), cos_ref[...], sin_ref[...])
        kv_own[:, cols] = key.astype(bf16)
    kv_own[:, KV_HEADS * width :] = v_ref[...]
    pl.semaphore_wait(barrier, count + 1)

    def ring_step(own, held, sends, recvs, t, p):
        cut = held.shape[1] // 2
        part = pl.ds(p * cut, cut)
        copies = []
        for way in range(2) if t < steps else (p,):
            slot = at(pos - (t - 1)) if way == 0 else at(pos + (t - 1))
            dst = held.at[slot].at[part]
            copies.append(
                send(
                    own.at[part] if t == 1 else dst,
                    dst,
                    sends.at[way, t - 1, p],
                    recvs.at[way, t - 1, p],
                    "sp",
                    behind if way else ahead,
                )
            )
            copies[-1].start()
        return copies

    kv_copies, w_copies = {}, {}

    def kv_step(t, p):
        kv_copies[t, p] = ring_step(kv_own, kv_all, kv_send, kv_recv, t, p)

    def w_step(t, p):
        w_copies[t, p] = ring_step(w_ref, w_all, w_send, w_recv, t, p)

    kv_step(1, 0)
    kv_step(1, 1)
    local = pltpu.make_async_copy(kv_own, kv_all.at[me], own_sem)
    local.start()
    for t in range(1, steps + 1):
        for p in range(2):
            for copy in kv_copies[t, p]:
                copy.wait_recv()
            if t < steps:
                kv_step(t + 1, p)
        if t == steps - 1:
            w_step(1, 0)
            w_step(1, 1)
    local.wait()

    def w_relay(t, p):
        for copy in w_copies[t, p]:
            copy.wait_recv()
        if t < steps:
            w_step(t + 1, p)

    allowed = lax.broadcasted_iota(jnp.int32, (rows, seqlen), 1) <= (
        me * rows + lax.broadcasted_iota(jnp.int32, (rows, seqlen), 0)
    )
    lane = lax.broadcasted_iota(jnp.int32, (rows, width), 1)

    def span(g):
        return pl.ds(pl.multiple_of(g * GROUP * VALUE_DIM, GROUP * VALUE_DIM), GROUP * VALUE_DIM)

    def sends_of(g):
        part = heads_all.at[d, :, span(g)]
        result = [send(part, part, x_send.at[0, g], x_recv.at[0, g], "dp", mate)]
        for k in range(1, half):
            result.append(send(part, part, x_send.at[k, g], x_recv.at[k, g], "dp", peer(k)))
        return result

    def one_group(g, carry):
        key = kv_all[:, :, pl.ds(pl.multiple_of(g * width, width), width)]
        key = key.reshape(seqlen, width)
        start = pl.multiple_of(KV_HEADS * width + g * VALUE_DIM, VALUE_DIM)
        value = kv_all[:, :, pl.ds(start, VALUE_DIM)].reshape(seqlen, VALUE_DIM)
        for h in range(GROUP):
            column = pl.multiple_of((g * GROUP + h) * width, width)
            query = q_ref[:, pl.ds(column, width)].astype(jnp.float32)
            query = turn(query, cos_ref[...], sin_ref[...]).astype(bf16)
            query = query.astype(jnp.float32) * HEAD_DIM**-0.5
            maps = []
            for m in range(2):
                mine = (lane < HEAD_DIM) if m == 0 else (lane >= HEAD_DIM)
                part = jnp.where(mine, query, 0.0).astype(bf16)
                scores = lax.dot_general(
                    part, key, (((1,), (1,)), ((), ())), preferred_element_type=jnp.float32
                )
                scores = jnp.where(allowed, scores, -1e30)
                raised = jnp.exp(scores - jnp.max(scores, -1, keepdims=True))
                maps.append((raised, 1.0 / jnp.sum(raised, -1, keepdims=True)))
            lam = lam_ref[g * GROUP + h]
            weights = (
                maps[0][0] * maps[0][1] - maps[1][0] * (lam * maps[1][1])
            ).astype(bf16)
            found = jnp.dot(weights, value, preferred_element_type=jnp.float32)
            squares = jnp.mean(found * found, -1, keepdims=True)
            normed = found * lax.rsqrt(squares + norm_eps) * gain_ref[...] * output_scale
            heads_all[d, :, pl.ds(column, width)] = normed.astype(bf16)
        for copy in sends_of(g):
            copy.start()
        return carry

    lax.fori_loop(0, KV_HEADS // 2, one_group, 0)
    w_relay(1, 0)
    lax.fori_loop(KV_HEADS // 2, KV_HEADS, one_group, 0)
    w_relay(1, 1)

    forwards = []
    for g in range(KV_HEADS):
        copies = sends_of(g)
        for k in range(1, half):
            copies[k].wait_recv()
            part = heads_all.at[(x + half - k) % half * 2 + core, :, span(g)]
            forwards.append(
                send(part, part, mate_send.at[k, g], mate_recv.at[k, g], "dp", mate)
            )
            forwards[-1].start()
    for g in range(KV_HEADS):
        sends_of(g)[0].wait_recv()
    for copy in forwards:
        copy.wait_recv()

    heads = heads_all[...].reshape(count * rows, heads_all.shape[2])
    own = w_ref.shape[1]
    outs = []

    def project(index, places):
        slots = [at(place) for place in places]
        blocks = [w_all[slot] if index else w_ref[...] for slot in slots]
        if own % 128 == 0:
            both = jnp.concatenate(blocks, -1) if len(blocks) > 1 else blocks[0]
            both = jnp.dot(heads, both, preferred_element_type=jnp.float32).astype(bf16)
            results = [both[:, i * own : (i + 1) * own] for i in range(len(blocks))]
        else:
            results = [
                jnp.dot(heads, block, preferred_element_type=jnp.float32).astype(bf16)
                for block in blocks
            ]
        for i in range(len(slots)):
            built[index, i] = results[i].reshape(count, rows, own)
        for k in range(1, count):
            to = (d + k) % count
            for i in range(len(slots)):
                outs.append(
                    send(
                        built.at[index, i, to],
                        out_ref.at[slots[i], d],
                        out_send.at[index, i, k],
                        out_recv.at[index, i, k],
                        "dp",
                        to,
                    )
                )
                outs[-1].start()
        for i in range(len(slots)):
            out_ref[slots[i], d] = built[index, i, d]

    project(0, (pos,))
    for t in range(1, steps + 1):
        if t > 1:
            w_relay(t, 0)
            w_relay(t, 1)
        project(t, (pos - t, pos + t) if t < steps else (pos + t,))
    for copy in outs:
        copy.wait()
    for copies in list(kv_copies.values()) + list(w_copies.values()):
        for copy in copies:
            copy.wait_send()
    for g in range(KV_HEADS):
        for copy in sends_of(g):
            copy.wait_send()
    for copy in forwards:
        copy.wait_send()


def lay_kernel(in_ref, out_ref):
    own = in_ref.shape[2]
    for b in range(in_ref.shape[0]):
        out_ref[:, b * own : (b + 1) * own] = in_ref[b]


def shards(queries, keys, values, lambdas, value_gain, out_weight):
    rows = queries.shape[1]
    sp_count = lax.axis_size("sp")
    dp_count = lax.axis_size("dp")
    width = 2 * HEAD_DIM
    vmem = pl.BlockSpec(memory_space=pltpu.VMEM)
    bf16 = jnp.bfloat16
    positions = (lax.axis_index("sp") * rows + jnp.arange(rows)).astype(jnp.float32)
    cosine, sine = tables(positions)
    kv_width = 2 * KV_HEADS * width

    half = dp_count // 2
    steps = sp_count // 2
    depth, own = out_weight.shape
    dma = pltpu.SemaphoreType.DMA
    mixed = pl.pallas_call(
        functools.partial(layer_kernel, sp_count, dp_count),
        out_shape=jax.ShapeDtypeStruct((sp_count, dp_count, rows, own), bf16),
        in_specs=[pl.BlockSpec(memory_space=pltpu.SMEM)] + [vmem] * 7,
        out_specs=vmem,
        scratch_shapes=[
            pltpu.VMEM((rows, kv_width), bf16),
            pltpu.VMEM((sp_count, rows, kv_width), bf16),
            pltpu.VMEM((sp_count, depth, own), bf16),
            pltpu.VMEM((dp_count, rows, depth), bf16),
            pltpu.VMEM((steps + 1, 2, dp_count, rows, own), bf16),
            dma(()),
        ]
        + [dma((2, steps, 2))] * 4
        + [dma((half, KV_HEADS))] * 4
        + [dma((steps + 1, 2, dp_count))] * 2,
        compiler_params=pltpu.CompilerParams(
            collective_id=0, has_side_effects=True, vmem_limit_bytes=60 * 2**20
        ),
        name="layer",
    )(lambdas, queries[0], keys[0], values[0], cosine, sine, value_gain[None], out_weight)

    if own % 128 == 0:
        return pl.pallas_call(
            lay_kernel,
            out_shape=jax.ShapeDtypeStruct((rows, sp_count * dp_count * own), bf16),
            in_specs=[vmem],
            out_specs=vmem,
            name="lay",
        )(mixed.reshape(-1, rows, own))[None]
    return jnp.transpose(mixed, (2, 0, 1, 3)).reshape(1, rows, -1)


def solution(mesh):
    return jax.shard_map(
        shards,
        mesh=mesh,
        in_specs=(
            P("dp", "sp", None),
            P("dp", "sp", None),
            P("dp", "sp", None),
            P(),
            P(),
            P(None, ("sp", "dp")),
        ),
        out_specs=P("dp", "sp", None),
        check_vma=False,
    )
```
